32 devices in a mesh: sp: 8 (over z, y), tp: 4 (over x, core).
Axes of the slice: x: 2, y: 2, z: 4, core: 2. Of those that a mesh axis runs over, the one named last changes fastest.
Arguments:
- tokens: bfloat16 [6144, 2048], P('sp', 'tp'), may hold values from -12 to 12
- query_weight: bfloat16 [2048, 1024], P('sp', 'tp'), may hold values from -0.176776695 to 0.176776695
- key_projection: bfloat16 [2048, 512], P('sp', 'tp'), may hold values from -0.176776695 to 0.176776695
- value_projection: bfloat16 [2048, 512], P('sp', 'tp'), may hold values from -0.125 to 0.125
- conv_in_weight: bfloat16 [2048, 1024], P('sp', 'tp'), may hold values from -0.125 to 0.125
- conv_gate_out: bfloat16 [2048, 1024], P('sp', 'tp'), may hold values from -0.125 to 0.125
- conv_gate_in: bfloat16 [2048, 1024], P('sp', 'tp'), may hold values from -0.125 to 0.125
- conv_taps: bfloat16 [3, 1024], P(None, 'tp'), may hold values from -3 to 3
- head_sink_logit: float32 [8], P('tp'), may hold values from 3 to 8
- out_attn_weight: bfloat16 [1024, 2048], P('tp', 'sp'), may hold values from -5 to 5
- out_conv_weight: bfloat16 [1024, 2048], P('tp', 'sp'), may hold values from -0.5 to 0.5
- out_gain: float32 [2048], P('tp'), may hold values from 0.1 to 1.9
Outputs:
- mixed: bfloat16 [6144, 2048], P('sp', 'tp')
The draws below stay inside these ranges and needn't reach their ends.
All inputs are finite; a program needn't handle non-finite values.
Results may differ from the reference program's by a relative error of at most 0.014.
Values may be sent and summed in bfloat16 or wider, within the bound.
A program may use at most 64 MiB of HBM per device.

```python
import jax
import jax.numpy as jnp
from jax import lax

MODEL_WIDTH = 2048
HEAD_SIZE = 128
QUERY_HEADS = 8
KEY_VALUE_HEADS = 4
CONV = 1024
WINDOW = 128
GRID = 64
TOKENS = 6144


def draw_tokens(key, part):
    base = jnp.clip(jax.random.normal(jax.random.fold_in(key, 3), (TOKENS, MODEL_WIDTH), jnp.float32), -6.0, 6.0)
    return jnp.clip(base, -12.0, 12.0).astype(jnp.bfloat16)


def query_key_pair(key):
    head_group = QUERY_HEADS // KEY_VALUE_HEADS
    limit_value = 8.0 * MODEL_WIDTH ** (-0.5)
    query_portion = jnp.clip(jax.random.normal(jax.random.fold_in(key, 21), (MODEL_WIDTH, KEY_VALUE_HEADS, head_group, HEAD_SIZE), jnp.float32), -6.0, 6.0)
    key_portion = jnp.clip(jax.random.normal(jax.random.fold_in(key, 22), (MODEL_WIDTH, KEY_VALUE_HEADS, 1, HEAD_SIZE), jnp.float32), -6.0, 6.0)
    query_matrix = jnp.clip(query_portion.reshape(MODEL_WIDTH, QUERY_HEADS * HEAD_SIZE) * MODEL_WIDTH ** (-0.5), -limit_value, limit_value)
    key_projected = jnp.clip(key_portion.reshape(MODEL_WIDTH, KEY_VALUE_HEADS * HEAD_SIZE) * MODEL_WIDTH ** (-0.5), -limit_value, limit_value)
    return (query_matrix, key_projected)


def draw_query_weight(key, part):
    return query_key_pair(key)[0].astype(jnp.bfloat16)


def draw_key_projection(key, part):
    return query_key_pair(key)[1].astype(jnp.bfloat16)


def out_block(key, salt, rows, factor, limit):
    base = jnp.clip(jax.random.normal(jax.random.fold_in(key, salt), (rows, MODEL_WIDTH), jnp.float32), -6.0, 6.0)
    common = 0.7 * jnp.clip(jax.random.normal(jax.random.fold_in(key, salt + 1), (rows, 1), jnp.float32), -6.0, 6.0)
    column = jnp.arange(MODEL_WIDTH, dtype=jnp.int32).astype(jnp.float32) / (MODEL_WIDTH - 1)
    exponent = column - 0.5
    scale = (10.0 ** exponent)[None, :]
    value_rows = (base + common) * scale * factor * rows ** (-0.5)
    return jnp.clip(value_rows, -limit * rows ** (-0.5), limit * rows ** (-0.5)).astype(jnp.bfloat16)


def draw_out_attn_weight(key, part):
    return out_block(key, 41, QUERY_HEADS * HEAD_SIZE, 5.0, 160.0)


def draw_out_conv_weight(key, part):
    return out_block(key, 51, CONV, 0.5, 16.0)


def shard_levels(rng, dims, cuts, smallest, largest):
    def one(dim, parts):
        steps = jax.random.uniform(jax.random.fold_in(jax.random.fold_in(rng, 6), dim), (parts,), jnp.float32, smallest / len(cuts), largest / len(cuts))
        return jnp.repeat(jnp.exp(steps), dims[dim] // parts).reshape((-1,) + (1,) * (len(dims) - dim - 1))

    factor_of = one(*cuts[0])
    for cut in cuts[1:]:
        factor_of = factor_of * one(*cut)
    return factor_of


def scatter_about(stream_key, dims, scale, most, shards=(), kind=jnp.bfloat16):
    array = scale * jax.random.normal(stream_key, dims, jnp.float32)
    if shards:
        array = array * shard_levels(stream_key, dims, shards, -0.22, 0.18)
    return jnp.clip(array, -most, most).astype(kind)


def setup_inputs(seed: int = 0) -> dict:
    key_list = jax.random.split(jax.random.key(seed), 13)
    return {
        "tokens": draw_tokens(jax.random.fold_in(key_list[12], 71), 0),
        "query_weight": draw_query_weight(jax.random.fold_in(key_list[12], 71), 0),
        "key_projection": draw_key_projection(jax.random.fold_in(key_list[12], 71), 0),
        "value_projection": scatter_about(key_list[3], (MODEL_WIDTH, KEY_VALUE_HEADS * HEAD_SIZE), MODEL_WIDTH ** -0.5, 0.125, ((0, 8), (1, 4))),
        "conv_in_weight": scatter_about(key_list[4], (MODEL_WIDTH, CONV), MODEL_WIDTH ** -0.5, 0.125, ((0, 8), (1, 4))),
        "conv_gate_out": scatter_about(key_list[5], (MODEL_WIDTH, CONV), MODEL_WIDTH ** -0.5, 0.125, ((0, 8), (1, 4))),
        "conv_gate_in": scatter_about(key_list[6], (MODEL_WIDTH, CONV), MODEL_WIDTH ** -0.5, 0.125, ((0, 8), (1, 4))),
        "conv_taps": scatter_about(key_list[7], (3, CONV), 0.6, 3.0, ((1, 4),)),
        "head_sink_logit": jnp.clip(3.0 + 5.0 * jax.random.uniform(key_list[8], (QUERY_HEADS,), jnp.float32) ** shard_levels(key_list[8], (QUERY_HEADS,), ((0, 4),), -0.2, 0.2), 3.0, 8.0),
        "out_attn_weight": draw_out_attn_weight(jax.random.fold_in(key_list[12], 71), 0),
        "out_conv_weight": draw_out_conv_weight(jax.random.fold_in(key_list[12], 71), 0),
        "out_gain": jnp.clip(1.0 + 0.18 * jax.random.normal(key_list[11], (MODEL_WIDTH,), jnp.float32), 0.1, 1.9),
    }


NEG_BIG = -1e+30
THETA = 10000.0
EPS = 1e-05

def rope_tables(positions):
    row = (positions // GRID).astype(jnp.float32)
    column = (positions % GRID).astype(jnp.float32)
    half = HEAD_SIZE // 2
    inverse = THETA ** (-jnp.arange(0, half, 2, dtype=jnp.float32) / half)
    angle_row = row[:, None] * inverse
    angle_col = column[:, None] * inverse
    angles = jnp.concatenate([angle_row, angle_row, angle_col, angle_col], -1)
    return (jnp.cos(angles)[:, None, :], jnp.sin(angles)[:, None, :])

def rotate(vectors, cosine, sine):
    first, second, third, fourth = jnp.split(vectors, 4, axis=-1)
    turned = jnp.concatenate([-second, first, -fourth, third], -1)
    return vectors * cosine + turned * sine

def band_head(inputs):
    query_vectors, key_rows, value_rows, sink = inputs
    item_count = query_vectors.shape[0]
    blocks = item_count // WINDOW

    def band(block):
        padded = jnp.pad(block, ((WINDOW, WINDOW), (0, 0))).reshape(blocks + 2, WINDOW, HEAD_SIZE)
        return jnp.concatenate([padded[:-2], padded[1:-1], padded[2:]], axis=1)
    query_blocks = query_vectors.reshape(blocks, WINDOW, -1, HEAD_SIZE).astype(jnp.float32)
    key_band = band(key_rows).astype(jnp.float32)
    value_band = band(value_rows).astype(jnp.float32)
    scores = jnp.einsum('nqgd,nkd->ngqk', query_blocks, key_band) * HEAD_SIZE ** (-0.5)
    block_start = jnp.arange(blocks, dtype=jnp.int32)[:, None] * WINDOW
    query_pos = block_start + jnp.arange(WINDOW, dtype=jnp.int32)[None, :]
    key_pos = block_start - WINDOW + jnp.arange(3 * WINDOW, dtype=jnp.int32)[None, :]
    distance = key_pos[:, None, :] - query_pos[:, :, None]
    valid = (jnp.abs(distance) <= WINDOW) & (key_pos[:, None, :] >= 0) & (key_pos[:, None, :] < item_count)
    scores = jnp.where(valid[:, None], scores, NEG_BIG)
    sink_col = sink.astype(jnp.float32).reshape(1, -1, 1, 1)
    top = jnp.maximum(lax.optimization_barrier(jnp.max(scores, -1, keepdims=True)), sink_col)
    weights = jnp.exp(scores - top)
    denominator = lax.optimization_barrier(jnp.sum(weights, -1, keepdims=True)) + jnp.exp(sink_col - top)
    probs = lax.optimization_barrier((weights / denominator).astype(jnp.bfloat16)).astype(jnp.float32)
    mixed = jnp.einsum('ngqk,nkd->nqgd', probs, value_band)
    return mixed.reshape(item_count, -1, HEAD_SIZE).astype(jnp.bfloat16)

def reference(tokens, query_weight, key_projection, value_projection, conv_in_weight, conv_gate_out, conv_gate_in, conv_taps, head_sink_logit, out_attn_weight, out_conv_weight, out_gain):
    item_count = tokens.shape[0]
    head_group = QUERY_HEADS // KEY_VALUE_HEADS
    positions = jnp.arange(item_count, dtype=jnp.int32)
    cosine, sine = rope_tables(positions)
    query_raw = jnp.dot(tokens, query_weight, preferred_element_type=jnp.float32).reshape(item_count, QUERY_HEADS, HEAD_SIZE)
    query_vectors = rotate(query_raw, cosine, sine).astype(jnp.bfloat16)
    key_unrotated = jnp.dot(tokens, key_projection, preferred_element_type=jnp.float32).reshape(item_count, KEY_VALUE_HEADS, HEAD_SIZE)
    key_rows = rotate(key_unrotated, cosine, sine).astype(jnp.bfloat16)
    value_rows = jnp.dot(tokens, value_projection, preferred_element_type=jnp.float32).astype(jnp.bfloat16)
    value_rows = value_rows.reshape(item_count, KEY_VALUE_HEADS, HEAD_SIZE)
    head_major = (jnp.transpose(query_vectors.reshape(item_count, KEY_VALUE_HEADS, head_group, HEAD_SIZE), (1, 0, 2, 3)), jnp.transpose(key_rows, (1, 0, 2)), jnp.transpose(value_rows, (1, 0, 2)), head_sink_logit.reshape(KEY_VALUE_HEADS, head_group))
    mixed_heads = lax.map(band_head, head_major)
    attention_out = jnp.transpose(mixed_heads, (1, 0, 2, 3)).reshape(item_count, QUERY_HEADS * HEAD_SIZE)
    conv_input = jnp.dot(tokens, conv_in_weight, preferred_element_type=jnp.float32)
    gate_after = jnp.dot(tokens, conv_gate_out, preferred_element_type=jnp.float32)
    gate_before = jnp.dot(tokens, conv_gate_in, preferred_element_type=jnp.float32)
    sectioned = (gate_before * conv_input).astype(jnp.bfloat16)
    padded = jnp.pad(sectioned, ((1, 1), (0, 0))).astype(jnp.float32)
    taps = conv_taps.astype(jnp.float32)
    conv_mix = padded[:-2] * taps[0] + padded[1:-1] * taps[1] + padded[2:] * taps[2]
    conv_out = (gate_after * conv_mix).astype(jnp.bfloat16)
    summed = jnp.dot(attention_out, out_attn_weight, preferred_element_type=jnp.float32) + jnp.dot(conv_out, out_conv_weight, preferred_element_type=jnp.float32)
    mean = lax.optimization_barrier(jnp.mean(summed, -1, keepdims=True))
    spread = lax.optimization_barrier(jnp.mean(jnp.square(summed - mean), -1, keepdims=True))
    return ((summed - mean) * lax.rsqrt(spread + EPS) * out_gain).astype(jnp.bfloat16)
```

```python
import functools

import jax
import jax.numpy as jnp
from jax import lax
from jax.experimental import pallas as pl
from jax.experimental.pallas import tpu as pltpu
from jax.sharding import PartitionSpec as P

HEAD_SIZE = 128
WINDOW = 128
GRID = 64


NEG_BIG = -1e30
THETA = 10000.0
EPS = 1e-05


def with_halo(block, sides, width):
    for axis, dim in sides:
        count = lax.axis_size(axis)
        forward = [(i, i + 1) for i in range(count - 1)]
        backward = [(target, source) for source, target in forward]
        low = lax.ppermute(
            lax.slice_in_dim(block, block.shape[dim] - width, None, axis=dim), axis, forward
        )
        high = lax.ppermute(lax.slice_in_dim(block, 0, width, axis=dim), axis, backward)
        block = jnp.concatenate([low, block, high], axis=dim)
    return block


def rope_tables(positions):
    row = (positions // GRID).astype(jnp.float32)
    column = (positions % GRID).astype(jnp.float32)
    half = HEAD_SIZE // 2
    inverse = THETA ** (-jnp.arange(0, half, 2, dtype=jnp.float32) / half)
    angle_row = row[:, None] * inverse
    angle_col = column[:, None] * inverse
    angles = jnp.concatenate([angle_row, angle_row, angle_col, angle_col], -1)
    return (jnp.cos(angles)[:, None, :], jnp.sin(angles)[:, None, :])


def rotate(vectors, cosine, sine):
    first, second, third, fourth = jnp.split(vectors, 4, axis=-1)
    turned = jnp.concatenate([-second, first, -fourth, third], -1)
    return vectors * cosine + turned * sine


def attend(query_vectors, paired, head_sink_logit, offset, total_tokens):
    item_count = query_vectors.shape[0]
    kv_heads = paired.shape[1] // (2 * HEAD_SIZE)
    head_group = query_vectors.shape[1] // (kv_heads * HEAD_SIZE)
    blocks = item_count // WINDOW
    padded = with_halo(paired, (("sp", 0),), WINDOW)
    shaped = padded.reshape(blocks + 2, WINDOW, paired.shape[1])
    banded = jnp.concatenate([shaped[:-2], shaped[1:-1], shaped[2:]], axis=1)
    banded = banded.reshape(blocks, 3 * WINDOW, 2, kv_heads, HEAD_SIZE)
    key_band = banded[:, :, 0]
    value_band = banded[:, :, 1]
    query_blocks = query_vectors.reshape(blocks, WINDOW, kv_heads, head_group, HEAD_SIZE)
    scores = jnp.einsum(
        "nqhgd,nkhd->nhgqk", query_blocks, key_band, preferred_element_type=jnp.float32
    ) * HEAD_SIZE ** (-0.5)
    block_start = offset + jnp.arange(blocks, dtype=jnp.int32)[:, None] * WINDOW
    query_pos = block_start + jnp.arange(WINDOW, dtype=jnp.int32)[None, :]
    key_pos = block_start - WINDOW + jnp.arange(3 * WINDOW, dtype=jnp.int32)[None, :]
    distance = key_pos[:, None, :] - query_pos[:, :, None]
    valid = (
        (jnp.abs(distance) <= WINDOW)
        & (key_pos[:, None, :] >= 0)
        & (key_pos[:, None, :] < total_tokens)
    )
    scores = jnp.where(valid[:, None, None], scores, NEG_BIG)
    sink_col = head_sink_logit.reshape(1, kv_heads, head_group, 1, 1)
    top = jnp.maximum(jnp.max(scores, -1, keepdims=True), sink_col)
    weights = jnp.exp(scores - top)
    denominator = jnp.sum(weights, -1, keepdims=True) + jnp.exp(sink_col - top)
    probs = (weights / denominator).astype(jnp.bfloat16)
    mixed_heads = jnp.einsum(
        "nhgqk,nkhd->nqhgd", probs, value_band, preferred_element_type=jnp.float32
    )
    return mixed_heads.reshape(item_count, kv_heads * head_group * HEAD_SIZE).astype(jnp.bfloat16)


def convolve(gate_before, conv_input, gate_after, conv_taps):
    sectioned = (gate_before * conv_input).astype(jnp.bfloat16)
    bordered = with_halo(sectioned, (("sp", 0),), 1)
    taps = conv_taps.astype(jnp.float32)
    conv_mix = bordered[:-2] * taps[0] + bordered[1:-1] * taps[1] + bordered[2:] * taps[2]
    return (gate_after * conv_mix).astype(jnp.bfloat16)


def plain_body(
    tokens,
    query_weight,
    key_projection,
    value_projection,
    conv_in_weight,
    conv_gate_out,
    conv_gate_in,
    conv_taps,
    head_sink_logit,
    out_attn_weight,
    out_conv_weight,
    out_gain,
):
    whole = lax.all_gather(tokens, "tp", axis=1, tiled=True)
    item_count = whole.shape[0]
    offset = lax.axis_index("sp") * item_count
    total_tokens = item_count * lax.axis_size("sp")
    positions = offset + jnp.arange(item_count, dtype=jnp.int32)
    cosine, sine = rope_tables(positions)
    pieces = (
        lax.all_gather(query_weight, "sp", axis=0, tiled=True),
        lax.all_gather(key_projection, "sp", axis=0, tiled=True),
        lax.all_gather(value_projection, "sp", axis=0, tiled=True),
        lax.all_gather(conv_in_weight, "sp", axis=0, tiled=True),
        lax.all_gather(conv_gate_out, "sp", axis=0, tiled=True),
        lax.all_gather(conv_gate_in, "sp", axis=0, tiled=True),
    )
    query_raw, key_unrotated, value_raw, conv_input, gate_after, gate_before = tuple(
        (jnp.dot(whole, piece, preferred_element_type=jnp.float32) for piece in pieces)
    )
    query_vectors = (
        rotate(query_raw.reshape(item_count, -1, HEAD_SIZE), cosine, sine)
        .reshape(item_count, -1)
        .astype(jnp.bfloat16)
    )
    key_rows = (
        rotate(key_unrotated.reshape(item_count, -1, HEAD_SIZE), cosine, sine)
        .reshape(item_count, -1)
        .astype(jnp.bfloat16)
    )
    paired = jnp.concatenate([key_rows, value_raw.astype(jnp.bfloat16)], 1)
    attention_out = attend(query_vectors, paired, head_sink_logit, offset, total_tokens)
    conv_out = convolve(gate_before, conv_input, gate_after, conv_taps)
    mixer_rows = jnp.concatenate([attention_out, conv_out], 1)
    stacked = jnp.concatenate([out_attn_weight, out_conv_weight], 0)
    own_width = out_gain.shape[0]
    partial_sums = jnp.dot(
        mixer_rows,
        lax.all_gather(stacked, "sp", axis=1, tiled=True),
        preferred_element_type=jnp.float32,
    )
    summed = lax.psum_scatter(
        partial_sums.astype(jnp.bfloat16), "tp", scatter_dimension=1, tiled=True
    ).astype(jnp.float32)
    full_width = own_width * lax.axis_size("tp")
    first_sum, square_sum = lax.psum((jnp.sum(summed, 1), jnp.sum(summed * summed, 1)), "tp")
    mean = first_sum / full_width
    spread = square_sum / full_width - mean * mean
    normed = (summed - mean[:, None]) * lax.rsqrt(spread[:, None] + EPS) * out_gain
    return normed.astype(jnp.bfloat16)


def fused_kernel(
    outer, tp, tokens_ref, wq_ref, wk_ref, wv_ref, wi_ref, wgo_ref, wgi_ref, wa_ref, wc_ref,
    taps_ref, sink_ref, gain_ref, cosr_ref, sinr_ref, cosc_ref, sinc_ref, out_ref,
    tok, a_buf, b_buf, c_buf, q_buf, kv, proj, sec, mix, stage, rbuf, loc, my_stat, stats,
    local_sem, w_send, w_recv, t_send, t_recv, halo_send, halo_recv, rs_send, rs_recv,
    st_send, st_recv,
):
    f32, bf16 = jnp.float32, jnp.bfloat16
    s, t = lax.axis_index("sp"), lax.axis_index("tp")
    span = 2 * outer
    o, i = lax.div(s, 2), lax.rem(s, 2)
    odd = lax.rem(o, 2)
    mate = o + 1 - 2 * odd
    partner = 2 * o + 1 - i
    items = tokens_ref.shape[0]
    blocks = items // WINDOW
    edge = 16
    sends = []
    always = s >= 0

    def remote(src, dst, send_sem, recv_sem, dev):
        return pltpu.make_async_remote_copy(
            src_ref=src, dst_ref=dst, send_sem=send_sem, recv_sem=recv_sem,
            device_id=dev, device_id_type=pl.DeviceIdType.MESH,
        )

    def post(cond, *args):
        def run():
            remote(*args).start()

        pl.when(cond)(run)
        sends.append((cond, args))

    half_c = wa_ref.shape[0]
    qw, kw = wq_ref.shape[1], wk_ref.shape[1]
    cw = wi_ref.shape[1]
    own = [
        (tokens_ref, tok.at[t]),
        (wq_ref, a_buf.at[s, :, pl.ds(0, qw)]),
        (wk_ref, a_buf.at[s, :, pl.ds(qw, kw)]),
        (wv_ref, a_buf.at[s, :, pl.ds(qw + kw, kw)]),
        (wi_ref, b_buf.at[s, :, pl.ds(0, cw)]),
        (wgo_ref, b_buf.at[s, :, pl.ds(cw, cw)]),
        (wgi_ref, b_buf.at[s, :, pl.ds(2 * cw, cw)]),
        (wa_ref, c_buf.at[s, pl.ds(0, half_c)]),
        (wc_ref, c_buf.at[s, pl.ds(half_c, half_c)]),
    ]
    local = [
        pltpu.make_async_copy(a, b, local_sem.at[n]) for n, (a, b) in enumerate(own)
    ]
    for copy in local:
        copy.start()

    barrier = pltpu.get_barrier_semaphore()
    greet = [(s + 1 < span, (s + 1, t)), (s > 0, (s - 1, t)),
             (o + 1 < outer, (s + 2, t)), (o > 0, (s - 2, t))]
    greet += [(always, (s, lax.rem(t + d, tp))) for d in range(1, tp)]
    for cond, dev in greet:
        @pl.when(cond)
        def _(dev=dev):
            pl.semaphore_signal(barrier, inc=1, device_id=dev, device_id_type=pl.DeviceIdType.MESH)
    pl.semaphore_wait(barrier, sum(cond.astype(jnp.int32) for cond, dev in greet))

    bufs = (a_buf, b_buf, c_buf)

    def unit(p, piece, h):
        rows = bufs[p].shape[1] // 2
        return bufs[p].at[piece, pl.ds(h * rows, rows)]

    def send(p, piece, h, d, dev, cond):
        ref = unit(p, piece, h)
        post(cond, ref, ref, w_send.at[p, d, piece, h], w_recv.at[p, piece, h], (dev, t))

    def recv(p, piece, h):
        ref = unit(p, piece, h)
        remote(ref, ref, w_send.at[p, 0, piece, h], w_recv.at[p, piece, h], (partner, t)).wait_recv()

    def step0(p):
        for h in range(2):
            send(p, s, h, 0, s + 2, o + 1 < outer)
            send(p, s, h, 1, s - 2, o > 0)
            send(p, s, h, 2, partner, always)

    def step0_partner(p):
        recv(p, partner, 0)
        recv(p, partner, 1)
        send(p, partner, 1, 3, 2 * mate + i, always)

    def step(p, k):
        for h in range(2):
            low, high = s - 2 * k, s + 2 * k
            has_low, has_high = o >= k, o + k < outer
            pl.when(has_low)(lambda: recv(p, low, h))
            send(p, low, h, 0, s + 2, has_low & (o + 1 < outer))
            skip = h == 1 and k == 1
            send(p, low, h, 2, partner, (has_low & (odd == 0)) if skip else has_low)
            pl.when(has_high)(lambda: recv(p, high, h))
            send(p, high, h, 1, s - 2, has_high & (o > 0))
            send(p, high, h, 2, partner, (has_high & (odd == 1)) if skip else has_high)

    def take(p, k, low):
        base = partner - 2 * k if low else partner + 2 * k
        for h in range(2):
            recv(p, base, h)

    def take_all(p):
        for k in range(1, outer):
            pl.when(o >= k)(lambda: take(p, k, True))
            pl.when(o + k < outer)(lambda: take(p, k, False))

    for copy in local[:4]:
        copy.wait()
    sibling = t + 1 - 2 * lax.rem(t, 2)
    post(always, tok.at[t], tok.at[t], t_send.at[0], t_recv.at[t], (s, sibling))
    across = [lax.rem(t + 2 * d, tp) for d in range(1, tp // 2)]
    for n, far in enumerate(across):
        post(always, tok.at[t], tok.at[t], t_send.at[1 + n], t_recv.at[t], (s, far))

    def wait_tok(src):
        remote(tok.at[src], tok.at[src], t_send.at[0], t_recv.at[src], (s, sibling)).wait_recv()

    step0(0)
    for copy in local[4:]:
        copy.wait()
    step0_partner(0)
    step(0, 1)
    step0(1)
    for k in range(2, outer):
        step(0, k)
    for n, far in enumerate(across):
        wait_tok(far)
        post(always, tok.at[far], tok.at[far], t_send.at[tp // 2 + n], t_recv.at[far], (s, sibling))
    wait_tok(sibling)
    for far in across:
        wait_tok(far + 1 - 2 * lax.rem(far, 2))
    take_all(0)

    tile = 256
    depth = a_buf.shape[1]
    per = tok.shape[2] // depth

    def project(buf, rows, cols):
        total = None
        for piece in range(span):
            lane = (piece % per) * depth
            term = jnp.dot(
                tok[piece // per, rows, lane : lane + depth], buf[piece, :, cols],
                preferred_element_type=f32,
            )
            total = term if total is None else total + term
        return total

    lane_row = lax.broadcasted_iota(jnp.int32, (1, HEAD_SIZE), 1)
    first_half = lax.rem(lane_row, HEAD_SIZE // 2) < HEAD_SIZE // 4
    left_lanes = (lane_row < HEAD_SIZE // 2)[None]
    for n in range(items // tile):
        rows = pl.ds(n * tile, tile)
        grid_rows = tile // GRID

        def table(row_ref, col_ref):
            r = row_ref[pl.ds(n * grid_rows, grid_rows), :][:, None, :]
            c = col_ref[...][None]
            r = jnp.broadcast_to(r, (grid_rows, GRID, HEAD_SIZE))
            c = jnp.broadcast_to(c, (grid_rows, GRID, HEAD_SIZE))
            return jnp.where(left_lanes, r, c).reshape(tile, HEAD_SIZE)

        cosine = table(cosr_ref, cosc_ref)
        sine = table(sinr_ref, sinc_ref)
        sine = jnp.where(first_half, -sine, sine)
        raw = project(a_buf, rows, slice(None))

        def turn(u):
            other = jnp.where(
                first_half, pltpu.roll(u, HEAD_SIZE - HEAD_SIZE // 4, 1), pltpu.roll(u, HEAD_SIZE // 4, 1)
            )
            return (u * cosine + other * sine).astype(bf16)

        for g in range(qw // HEAD_SIZE):
            cols = slice(g * HEAD_SIZE, (g + 1) * HEAD_SIZE)
            q_buf[rows, cols] = turn(raw[:, cols])
        inner = pl.ds(WINDOW + n * tile, tile)
        kv[inner, :kw] = turn(raw[:, qw : qw + kw])
        kv[inner, kw:] = raw[:, qw + kw :].astype(bf16)

    has_left, has_right = s > 0, s + 1 < span

    def halo(ref, width, base):
        last = ref.shape[0] - width
        post(has_right, ref.at[pl.ds(last - width, width)], ref.at[pl.ds(0, width)],
             halo_send.at[base], halo_recv.at[base], (s + 1, t))
        post(has_left, ref.at[pl.ds(width, width)], ref.at[pl.ds(last, width)],
             halo_send.at[base + 1], halo_recv.at[base + 1], (s - 1, t))

    def halo_wait(ref, width, base):
        last = ref.shape[0] - width
        for n, (cond, start) in enumerate(((has_left, 0), (has_right, last))):
            dst = ref.at[pl.ds(start, width)]

            @pl.when(cond)
            def _():
                remote(dst, dst, halo_send.at[base + n], halo_recv.at[base + n], (partner, t)).wait_recv()

            @pl.when(jnp.logical_not(cond))
            def _():
                ref[pl.ds(start, width), :] = jnp.zeros((width, ref.shape[1]), ref.dtype)

    halo(kv, WINDOW, 0)

    group = qw // HEAD_SIZE
    shape = (group * WINDOW, 3 * WINDOW)

    def attend_block(b):
        rows = pl.ds(b * WINDOW, WINDOW)
        band = pl.ds(b * WINDOW, 3 * WINDOW)
        q = jnp.concatenate(
            [q_buf[rows, g * HEAD_SIZE : (g + 1) * HEAD_SIZE] for g in range(group)], 0
        )
        scores = lax.dot_general(
            q, kv[band, :kw], (((1,), (1,)), ((), ())), preferred_element_type=f32
        ) * HEAD_SIZE ** (-0.5)
        row = lax.broadcasted_iota(jnp.int32, shape, 0)
        col = lax.broadcasted_iota(jnp.int32, shape, 1)
        gap = col - WINDOW - lax.rem(row, WINDOW)
        position = s * items + (b - 1) * WINDOW + col
        valid = (jnp.abs(gap) <= WINDOW) & (position >= 0) & (position < items * span)
        scores = jnp.where(valid, scores, NEG_BIG)
        head = lax.broadcasted_iota(jnp.int32, (group * WINDOW, 1), 0) // WINDOW
        sink = jnp.zeros((group * WINDOW, 1), f32)
        for g in range(group):
            sink = jnp.where(head == g, sink_ref[g], sink)
        top = jnp.maximum(jnp.max(scores, -1, keepdims=True), sink)
        weights = jnp.exp(scores - top)
        denominator = jnp.sum(weights, -1, keepdims=True) + jnp.exp(sink - top)
        probs = (weights / denominator).astype(bf16)
        mixed = jnp.dot(probs, kv[band, kw:], preferred_element_type=f32).astype(bf16)
        for g in range(group):
            mix[rows, g * HEAD_SIZE : (g + 1) * HEAD_SIZE] = mixed[g * WINDOW : (g + 1) * WINDOW]

    step0_partner(1)
    step(1, 1)
    for b in range(1, blocks - 1):
        attend_block(b)
    step(1, 2) if outer > 2 else None
    step0(2)
    halo_wait(kv, WINDOW, 0)
    attend_block(0)
    attend_block(blocks - 1)
    for k in range(3, outer):
        step(1, k)
    take_all(1)

    for n in range(items // tile):
        rows = pl.ds(n * tile, tile)
        inner = pl.ds(edge + n * tile, tile)
        conv_input = project(b_buf, rows, slice(0, cw))
        before = project(b_buf, rows, slice(2 * cw, 3 * cw))
        sec[inner, :] = (before * conv_input).astype(bf16)
    halo(sec, edge, 2)
    for n in range(items // tile):
        rows = pl.ds(n * tile, tile)
        proj[rows, :] = project(b_buf, rows, slice(cw, 2 * cw))
    step0_partner(2)
    step(2, 1)
    halo_wait(sec, edge, 2)
    full = sec[...].astype(f32)
    taps = taps_ref[...].astype(f32)
    length = full.shape[0]
    conv = (
        pltpu.roll(full, 1, 0) * taps[0:1]
        + full * taps[1:2]
        + pltpu.roll(full, length - 1, 0) * taps[2:3]
    )
    mix[:, qw:] = (proj[...] * conv[edge : edge + items]).astype(bf16)

    width = c_buf.shape[2]

    def produce(owner):
        def one(n, carry):
            rows = pl.ds(pl.multiple_of(n * tile, tile), tile)
            x = mix[rows, :]
            for j in range(2):
                y = jnp.dot(x, c_buf[2 * owner + j], preferred_element_type=f32)
                stage[owner, rows, j * width : (j + 1) * width] = y.astype(bf16)

                @pl.when(owner == t)
                def _():
                    loc[rows, j * width : (j + 1) * width] = y
            return carry

        lax.fori_loop(0, items // tile, one, 0)

    def give(cond, owner):
        pl.when(cond)(lambda: produce(owner))
        post(cond & (owner != t), stage.at[owner], rbuf.at[t], rs_send.at[owner], rs_recv.at[t], (s, owner))

    give(always, o)
    for k in range(1, outer):
        if k > 1:
            step(2, k)
        pl.when(o >= k)(lambda: take(2, k, True))
        pl.when(o + k < outer)(lambda: take(2, k, False))
        give(o >= k, o - k)
        give(o + k < outer, o + k)

    summed = loc[...]
    for d in range(1, tp):
        src = lax.rem(t + d, tp)
        remote(rbuf.at[src], rbuf.at[src], rs_send.at[0], rs_recv.at[src], (s, src)).wait_recv()
        summed = summed + rbuf[src].astype(f32)
    loc[...] = summed
    lane = lax.broadcasted_iota(jnp.int32, (items, 128), 1)
    both = jnp.where(
        lane == 0, jnp.sum(summed, 1, keepdims=True), jnp.sum(summed * summed, 1, keepdims=True)
    )
    my_stat[...] = jnp.transpose(both)[:8]
    for d in range(1, tp):
        dst = lax.rem(t + d, tp)
        post(always, my_stat, stats.at[t], st_send.at[d], st_recv.at[t], (s, dst))
    total = my_stat[...]
    for d in range(1, tp):
        src = lax.rem(t + d, tp)
        remote(stats.at[src], stats.at[src], st_send.at[0], st_recv.at[src], (s, src)).wait_recv()
        total = total + stats[src]
    total = total * (1.0 / (tp * out_ref.shape[1]))
    total = jnp.transpose(jnp.concatenate([total] * 16, 0))
    mean = total[:, 0:1]
    spread = total[:, 1:2] - mean * mean
    out_ref[...] = ((loc[...] - mean) * lax.rsqrt(spread + EPS) * gain_ref[...]).astype(bf16)

    for cond, args in sends:
        pl.when(cond)(lambda args=args: remote(*args).wait_send())


def small_tables(offset, items):
    half = HEAD_SIZE // 2
    inverse = THETA ** (-jnp.arange(0, half, 2, dtype=jnp.float32) / half)
    inverse = jnp.concatenate([inverse] * 4)[None]
    row = (offset // GRID + jnp.arange(items // GRID, dtype=jnp.int32)).astype(jnp.float32)
    column = jnp.arange(GRID, dtype=jnp.int32).astype(jnp.float32)
    row, column = row[:, None] * inverse, column[:, None] * inverse
    return jnp.cos(row), jnp.sin(row), jnp.cos(column), jnp.sin(column)


def body(
    sizes, tokens, query_weight, key_projection, value_projection, conv_in_weight, conv_gate_out,
    conv_gate_in, conv_taps, head_sink_logit, out_attn_weight, out_conv_weight, out_gain,
):
    span, tp = sizes["sp"], sizes["tp"]
    items, features = tokens.shape
    depth = query_weight.shape[0]
    group = query_weight.shape[1] // HEAD_SIZE
    fits = (
        span == 2 * tp and tp % 2 == 0 and depth % 128 == 0 and features == 2 * depth
        and out_attn_weight.shape[1] % 128 == 0 and items % (2 * WINDOW) == 0
        and key_projection.shape[1] == HEAD_SIZE and conv_in_weight.shape[1] % 128 == 0
        and out_attn_weight.shape[0] == out_conv_weight.shape[0]
    )
    if not fits:
        return plain_body(
            tokens, query_weight, key_projection, value_projection, conv_in_weight, conv_gate_out,
            conv_gate_in, conv_taps, head_sink_logit, out_attn_weight, out_conv_weight, out_gain,
        )
    tables = small_tables(lax.axis_index("sp") * items, items)
    outer = span // 2
    f32, bf16 = jnp.float32, jnp.bfloat16
    qw, kw, cw = query_weight.shape[1], key_projection.shape[1], conv_in_weight.shape[1]
    mixer = out_attn_weight.shape[0] + out_conv_weight.shape[0]
    own_width = out_gain.shape[0]
    dma = pltpu.SemaphoreType.DMA
    anywhere = pl.BlockSpec(memory_space=pl.ANY)
    vmem = pl.BlockSpec(memory_space=pltpu.VMEM)
    smem = pl.BlockSpec(memory_space=pltpu.SMEM)
    return pl.pallas_call(
        functools.partial(fused_kernel, outer, tp),
        out_shape=jax.ShapeDtypeStruct((items, own_width), bf16),
        in_specs=[anywhere] * 9 + [vmem, smem, vmem] + [vmem] * 4,
        out_specs=vmem,
        scratch_shapes=[
            pltpu.VMEM((tp, items, features), bf16),
            pltpu.VMEM((span, depth, qw + 2 * kw), bf16),
            pltpu.VMEM((span, depth, 3 * cw), bf16),
            pltpu.VMEM((span, mixer, out_attn_weight.shape[1]), bf16),
            pltpu.VMEM((items, qw), bf16),
            pltpu.VMEM((items + 2 * WINDOW, 2 * kw), bf16),
            pltpu.VMEM((items, cw), f32),
            pltpu.VMEM((items + 32, cw), bf16),
            pltpu.VMEM((items, mixer), bf16),
            pltpu.VMEM((tp, items, own_width), bf16),
            pltpu.VMEM((tp, items, own_width), bf16),
            pltpu.VMEM((items, own_width), f32),
            pltpu.VMEM((8, items), f32),
            pltpu.VMEM((tp, 8, items), f32),
            dma((9,)),
            dma((3, 4, span, 2)),
            dma((3, span, 2)),
            dma((tp,)),
            dma((tp,)),
            dma((4,)),
            dma((4,)),
            dma((tp,)),
            dma((tp,)),
            dma((tp,)),
            dma((tp,)),
        ],
        compiler_params=pltpu.CompilerParams(
            collective_id=0, has_side_effects=True, vmem_limit_bytes=60 * 2**20
        ),
    )(
        tokens, query_weight, key_projection, value_projection, conv_in_weight, conv_gate_out,
        conv_gate_in, out_attn_weight, out_conv_weight, conv_taps, head_sink_logit,
        out_gain[None], *tables,
    )


def solution(mesh):
    return jax.shard_map(
        functools.partial(body, dict(mesh.shape)),
        mesh=mesh,
        in_specs=(
            P("sp", "tp"),
            P("sp", "tp"),
            P("sp", "tp"),
            P("sp", "tp"),
            P("sp", "tp"),
            P("sp", "tp"),
            P("sp", "tp"),
            P(None, "tp"),
            P("tp"),
            P("tp", "sp"),
            P("tp", "sp"),
            P("tp"),
        ),
        out_specs=P("sp", "tp"),
        check_vma=False,
    )
```

```python
import functools

import jax
import jax.numpy as jnp
from jax import lax
from jax.experimental import pallas as pl
from jax.experimental.pallas import tpu as pltpu
from jax.sharding import PartitionSpec as P

HEAD_SIZE = 128
WINDOW = 128
GRID = 64


NEG_BIG = -1e30
THETA = 10000.0
EPS = 1e-05


def with_halo(block, sides, width):
    for axis, dim in sides:
        count = lax.axis_size(axis)
        forward = [(i, i + 1) for i in range(count - 1)]
        backward = [(target, source) for source, target in forward]
        low = lax.ppermute(
            lax.slice_in_dim(block, block.shape[dim] - width, None, axis=dim), axis, forward
        )
        high = lax.ppermute(lax.slice_in_dim(block, 0, width, axis=dim), axis, backward)
        block = jnp.concatenate([low, block, high], axis=dim)
    return block


def rope_tables(positions):
    row = (positions // GRID).astype(jnp.float32)
    column = (positions % GRID).astype(jnp.float32)
    half = HEAD_SIZE // 2
    inverse = THETA ** (-jnp.arange(0, half, 2, dtype=jnp.float32) / half)
    angle_row = row[:, None] * inverse
    angle_col = column[:, None] * inverse
    angles = jnp.concatenate([angle_row, angle_row, angle_col, angle_col], -1)
    return (jnp.cos(angles)[:, None, :], jnp.sin(angles)[:, None, :])


def rotate(vectors, cosine, sine):
    first, second, third, fourth = jnp.split(vectors, 4, axis=-1)
    turned = jnp.concatenate([-second, first, -fourth, third], -1)
    return vectors * cosine + turned * sine


def attend(query_vectors, paired, head_sink_logit, offset, total_tokens):
    item_count = query_vectors.shape[0]
    kv_heads = paired.shape[1] // (2 * HEAD_SIZE)
    head_group = query_vectors.shape[1] // (kv_heads * HEAD_SIZE)
    blocks = item_count // WINDOW
    padded = with_halo(paired, (("sp", 0),), WINDOW)
    shaped = padded.reshape(blocks + 2, WINDOW, paired.shape[1])
    banded = jnp.concatenate([shaped[:-2], shaped[1:-1], shaped[2:]], axis=1)
    banded = banded.reshape(blocks, 3 * WINDOW, 2, kv_heads, HEAD_SIZE)
    key_band = banded[:, :, 0]
    value_band = banded[:, :, 1]
    query_blocks = query_vectors.reshape(blocks, WINDOW, kv_heads, head_group, HEAD_SIZE)
    scores = jnp.einsum(
        "nqhgd,nkhd->nhgqk", query_blocks, key_band, preferred_element_type=jnp.float32
    ) * HEAD_SIZE ** (-0.5)
    block_start = offset + jnp.arange(blocks, dtype=jnp.int32)[:, None] * WINDOW
    query_pos = block_start + jnp.arange(WINDOW, dtype=jnp.int32)[None, :]
    key_pos = block_start - WINDOW + jnp.arange(3 * WINDOW, dtype=jnp.int32)[None, :]
    distance = key_pos[:, None, :] - query_pos[:, :, None]
    valid = (
        (jnp.abs(distance) <= WINDOW)
        & (key_pos[:, None, :] >= 0)
        & (key_pos[:, None, :] < total_tokens)
    )
    scores = jnp.where(valid[:, None, None], scores, NEG_BIG)
    sink_col = head_sink_logit.reshape(1, kv_heads, head_group, 1, 1)
    top = jnp.maximum(jnp.max(scores, -1, keepdims=True), sink_col)
    weights = jnp.exp(scores - top)
    denominator = jnp.sum(weights, -1, keepdims=True) + jnp.exp(sink_col - top)
    probs = (weights / denominator).astype(jnp.bfloat16)
    mixed_heads = jnp.einsum(
        "nhgqk,nkhd->nqhgd", probs, value_band, preferred_element_type=jnp.float32
    )
    return mixed_heads.reshape(item_count, kv_heads * head_group * HEAD_SIZE).astype(jnp.bfloat16)


def convolve(gate_before, conv_input, gate_after, conv_taps):
    sectioned = (gate_before * conv_input).astype(jnp.bfloat16)
    bordered = with_halo(sectioned, (("sp", 0),), 1)
    taps = conv_taps.astype(jnp.float32)
    conv_mix = bordered[:-2] * taps[0] + bordered[1:-1] * taps[1] + bordered[2:] * taps[2]
    return (gate_after * conv_mix).astype(jnp.bfloat16)


def plain_body(
    tokens,
    query_weight,
    key_projection,
    value_projection,
    conv_in_weight,
    conv_gate_out,
    conv_gate_in,
    conv_taps,
    head_sink_logit,
    out_attn_weight,
    out_conv_weight,
    out_gain,
):
    whole = lax.all_gather(tokens, "tp", axis=1, tiled=True)
    item_count = whole.shape[0]
    offset = lax.axis_index("sp") * item_count
    total_tokens = item_count * lax.axis_size("sp")
    positions = offset + jnp.arange(item_count, dtype=jnp.int32)
    cosine, sine = rope_tables(positions)
    pieces = (
        lax.all_gather(query_weight, "sp", axis=0, tiled=True),
        lax.all_gather(key_projection, "sp", axis=0, tiled=True),
        lax.all_gather(value_projection, "sp", axis=0, tiled=True),
        lax.all_gather(conv_in_weight, "sp", axis=0, tiled=True),
        lax.all_gather(conv_gate_out, "sp", axis=0, tiled=True),
        lax.all_gather(conv_gate_in, "sp", axis=0, tiled=True),
    )
    query_raw, key_unrotated, value_raw, conv_input, gate_after, gate_before = tuple(
        (jnp.dot(whole, piece, preferred_element_type=jnp.float32) for piece in pieces)
    )
    query_vectors = (
        rotate(query_raw.reshape(item_count, -1, HEAD_SIZE), cosine, sine)
        .reshape(item_count, -1)
        .astype(jnp.bfloat16)
    )
    key_rows = (
        rotate(key_unrotated.reshape(item_count, -1, HEAD_SIZE), cosine, sine)
        .reshape(item_count, -1)
        .astype(jnp.bfloat16)
    )
    paired = jnp.concatenate([key_rows, value_raw.astype(jnp.bfloat16)], 1)
    attention_out = attend(query_vectors, paired, head_sink_logit, offset, total_tokens)
    conv_out = convolve(gate_before, conv_input, gate_after, conv_taps)
    mixer_rows = jnp.concatenate([attention_out, conv_out], 1)
    stacked = jnp.concatenate([out_attn_weight, out_conv_weight], 0)
    own_width = out_gain.shape[0]
    partial_sums = jnp.dot(
        mixer_rows,
        lax.all_gather(stacked, "sp", axis=1, tiled=True),
        preferred_element_type=jnp.float32,
    )
    summed = lax.psum_scatter(
        partial_sums.astype(jnp.bfloat16), "tp", scatter_dimension=1, tiled=True
    ).astype(jnp.float32)
    full_width = own_width * lax.axis_size("tp")
    first_sum, square_sum = lax.psum((jnp.sum(summed, 1), jnp.sum(summed * summed, 1)), "tp")
    mean = first_sum / full_width
    spread = square_sum / full_width - mean * mean
    normed = (summed - mean[:, None]) * lax.rsqrt(spread[:, None] + EPS) * out_gain
    return normed.astype(jnp.bfloat16)


def fused_kernel(
    outer, tp, tokens_ref, wq_ref, wk_ref, wv_ref, wi_ref, wgo_ref, wgi_ref, wa_ref, wc_ref,
    taps_ref, sink_ref, gain_ref, cosr_ref, sinr_ref, cosc_ref, sinc_ref, out_ref,
    tok, a_buf, b_buf, c_buf, q_buf, kv, proj, sec, mix, stage, rbuf, pair, pre, loc, my_stat, stats,
    local_sem, w_send, w_recv, t_send, t_recv, halo_send, halo_recv, rs_send, rs_recv, pair_recv,
    st_send, st_recv,
):
    f32, bf16 = jnp.float32, jnp.bfloat16
    s, t = lax.axis_index("sp"), lax.axis_index("tp")
    span = 2 * outer
    o, i = lax.div(s, 2), lax.rem(s, 2)
    odd = lax.rem(o, 2)
    mate = o + 1 - 2 * odd
    partner = 2 * o + 1 - i
    items = tokens_ref.shape[0]
    blocks = items // WINDOW
    edge = 16
    sends = []
    always = s >= 0

    def remote(src, dst, send_sem, recv_sem, dev):
        return pltpu.make_async_remote_copy(
            src_ref=src, dst_ref=dst, send_sem=send_sem, recv_sem=recv_sem,
            device_id=dev, device_id_type=pl.DeviceIdType.MESH,
        )

    def post(cond, *args):
        def run():
            remote(*args).start()

        pl.when(cond)(run)
        sends.append((cond, args))

    half_c = wa_ref.shape[0]
    qw, kw = wq_ref.shape[1], wk_ref.shape[1]
    cw = wi_ref.shape[1]
    own = [
        (tokens_ref, tok.at[t]),
        (wq_ref, a_buf.at[s, :, pl.ds(0, qw)]),
        (wk_ref, a_buf.at[s, :, pl.ds(qw, kw)]),
        (wv_ref, a_buf.at[s, :, pl.ds(qw + kw, kw)]),
        (wi_ref, b_buf.at[s, :, pl.ds(0, cw)]),
        (wgo_ref, b_buf.at[s, :, pl.ds(cw, cw)]),
        (wgi_ref, b_buf.at[s, :, pl.ds(2 * cw, cw)]),
        (wa_ref, c_buf.at[s, pl.ds(0, half_c)]),
        (wc_ref, c_buf.at[s, pl.ds(half_c, half_c)]),
    ]
    local = [
        pltpu.make_async_copy(a, b, local_sem.at[n]) for n, (a, b) in enumerate(own)
    ]
    for copy in local:
        copy.start()

    barrier = pltpu.get_barrier_semaphore()
    greet = [(s + 1 < span, (s + 1, t)), (s > 0, (s - 1, t)),
             (o + 1 < outer, (s + 2, t)), (o > 0, (s - 2, t))]
    greet += [(always, (s, lax.rem(t + d, tp))) for d in range(1, tp)]
    for cond, dev in greet:
        @pl.when(cond)
        def _(dev=dev):
            pl.semaphore_signal(barrier, inc=1, device_id=dev, device_id_type=pl.DeviceIdType.MESH)
    pl.semaphore_wait(barrier, sum(cond.astype(jnp.int32) for cond, dev in greet))

    bufs = (a_buf, b_buf, c_buf)

    def unit(p, piece, h):
        rows = bufs[p].shape[1] // 2
        return bufs[p].at[piece, pl.ds(h * rows, rows)]

    def send(p, piece, h, d, dev, cond):
        ref = unit(p, piece, h)
        post(cond, ref, ref, w_send.at[p, d, piece, h], w_recv.at[p, piece, h], (dev, t))

    def recv(p, piece, h):
        ref = unit(p, piece, h)
        remote(ref, ref, w_send.at[p, 0, piece, h], w_recv.at[p, piece, h], (partner, t)).wait_recv()

    def step0(p):
        for h in range(2):
            send(p, s, h, 0, s + 2, o + 1 < outer)
            send(p, s, h, 1, s - 2, o > 0)
            send(p, s, h, 2, partner, always)

    def step0_partner(p):
        recv(p, partner, 0)
        recv(p, partner, 1)
        send(p, partner, 1, 3, 2 * mate + i, always)

    def step(p, k):
        for h in range(2):
            low, high = s - 2 * k, s + 2 * k
            has_low, has_high = o >= k, o + k < outer
            pl.when(has_low)(lambda: recv(p, low, h))
            send(p, low, h, 0, s + 2, has_low & (o + 1 < outer))
            skip = h == 1 and k == 1
            send(p, low, h, 2, partner, (has_low & (odd == 0)) if skip else has_low)
            pl.when(has_high)(lambda: recv(p, high, h))
            send(p, high, h, 1, s - 2, has_high & (o > 0))
            send(p, high, h, 2, partner, (has_high & (odd == 1)) if skip else has_high)

    def take(p, k, low):
        base = partner - 2 * k if low else partner + 2 * k
        for h in range(2):
            recv(p, base, h)

    def take_all(p):
        for k in range(1, outer):
            pl.when(o >= k)(lambda: take(p, k, True))
            pl.when(o + k < outer)(lambda: take(p, k, False))

    for copy in local[:4]:
        copy.wait()
    sibling = t + 1 - 2 * lax.rem(t, 2)
    post(always, tok.at[t], tok.at[t], t_send.at[0], t_recv.at[t], (s, sibling))
    across = [lax.rem(t + 2 * d, tp) for d in range(1, tp // 2)]
    for n, far in enumerate(across):
        post(always, tok.at[t], tok.at[t], t_send.at[1 + n], t_recv.at[t], (s, far))

    def wait_tok(src):
        remote(tok.at[src], tok.at[src], t_send.at[0], t_recv.at[src], (s, sibling)).wait_recv()

    step0(0)
    for copy in local[4:]:
        copy.wait()
    step0_partner(0)
    step(0, 1)
    step0(1)
    for k in range(2, outer):
        step(0, k)
    for n, far in enumerate(across):
        wait_tok(far)
        post(always, tok.at[far], tok.at[far], t_send.at[tp // 2 + n], t_recv.at[far], (s, sibling))
    wait_tok(sibling)
    for far in across:
        wait_tok(far + 1 - 2 * lax.rem(far, 2))
    take_all(0)

    tile = 256
    depth = a_buf.shape[1]
    per = tok.shape[2] // depth

    def project(buf, rows, cols):
        total = None
        for piece in range(span):
            lane = (piece % per) * depth
            term = jnp.dot(
                tok[piece // per, rows, lane : lane + depth], buf[piece, :, cols],
                preferred_element_type=f32,
            )
            total = term if total is None else total + term
        return total

    lane_row = lax.broadcasted_iota(jnp.int32, (1, HEAD_SIZE), 1)
    first_half = lax.rem(lane_row, HEAD_SIZE // 2) < HEAD_SIZE // 4
    left_lanes = (lane_row < HEAD_SIZE // 2)[None]
    for n in range(items // tile):
        rows = pl.ds(n * tile, tile)
        grid_rows = tile // GRID

        def table(row_ref, col_ref):
            r = row_ref[pl.ds(n * grid_rows, grid_rows), :][:, None, :]
            c = col_ref[...][None]
            r = jnp.broadcast_to(r, (grid_rows, GRID, HEAD_SIZE))
            c = jnp.broadcast_to(c, (grid_rows, GRID, HEAD_SIZE))
            return jnp.where(left_lanes, r, c).reshape(tile, HEAD_SIZE)

        cosine = table(cosr_ref, cosc_ref)
        sine = table(sinr_ref, sinc_ref)
        sine = jnp.where(first_half, -sine, sine)
        raw = project(a_buf, rows, slice(None))

        def turn(u):
            other = jnp.where(
                first_half, pltpu.roll(u, HEAD_SIZE - HEAD_SIZE // 4, 1), pltpu.roll(u, HEAD_SIZE // 4, 1)
            )
            return (u * cosine + other * sine).astype(bf16)

        for g in range(qw // HEAD_SIZE):
            cols = slice(g * HEAD_SIZE, (g + 1) * HEAD_SIZE)
            q_buf[rows, cols] = turn(raw[:, cols])
        inner = pl.ds(WINDOW + n * tile, tile)
        kv[inner, :kw] = turn(raw[:, qw : qw + kw])
        kv[inner, kw:] = raw[:, qw + kw :].astype(bf16)

    has_left, has_right = s > 0, s + 1 < span

    def halo(ref, width, base):
        last = ref.shape[0] - width
        post(has_right, ref.at[pl.ds(last - width, width)], ref.at[pl.ds(0, width)],
             halo_send.at[base], halo_recv.at[base], (s + 1, t))
        post(has_left, ref.at[pl.ds(width, width)], ref.at[pl.ds(last, width)],
             halo_send.at[base + 1], halo_recv.at[base + 1], (s - 1, t))

    def halo_wait(ref, width, base):
        last = ref.shape[0] - width
        for n, (cond, start) in enumerate(((has_left, 0), (has_right, last))):
            dst = ref.at[pl.ds(start, width)]

            @pl.when(cond)
            def _():
                remote(dst, dst, halo_send.at[base + n], halo_recv.at[base + n], (partner, t)).wait_recv()

            @pl.when(jnp.logical_not(cond))
            def _():
                ref[pl.ds(start, width), :] = jnp.zeros((width, ref.shape[1]), ref.dtype)

    halo(kv, WINDOW, 0)

    group = qw // HEAD_SIZE
    shape = (group * WINDOW, 3 * WINDOW)

    def attend_block(b):
        rows = pl.ds(b * WINDOW, WINDOW)
        band = pl.ds(b * WINDOW, 3 * WINDOW)
        q = jnp.concatenate(
            [q_buf[rows, g * HEAD_SIZE : (g + 1) * HEAD_SIZE] for g in range(group)], 0
        )
        scores = lax.dot_general(
            q, kv[band, :kw], (((1,), (1,)), ((), ())), preferred_element_type=f32
        ) * HEAD_SIZE ** (-0.5)
        row = lax.broadcasted_iota(jnp.int32, shape, 0)
        col = lax.broadcasted_iota(jnp.int32, shape, 1)
        gap = col - WINDOW - lax.rem(row, WINDOW)
        position = s * items + (b - 1) * WINDOW + col
        valid = (jnp.abs(gap) <= WINDOW) & (position >= 0) & (position < items * span)
        scores = jnp.where(valid, scores, NEG_BIG)
        head = lax.broadcasted_iota(jnp.int32, (group * WINDOW, 1), 0) // WINDOW
        sink = jnp.zeros((group * WINDOW, 1), f32)
        for g in range(group):
            sink = jnp.where(head == g, sink_ref[g], sink)
        top = jnp.maximum(jnp.max(scores, -1, keepdims=True), sink)
        weights = jnp.exp(scores - top)
        denominator = jnp.sum(weights, -1, keepdims=True) + jnp.exp(sink - top)
        probs = (weights / denominator).astype(bf16)
        mixed = jnp.dot(probs, kv[band, kw:], preferred_element_type=f32).astype(bf16)
        for g in range(group):
            mix[rows, g * HEAD_SIZE : (g + 1) * HEAD_SIZE] = mixed[g * WINDOW : (g + 1) * WINDOW]

    step0_partner(1)
    step(1, 1)
    for b in range(1, blocks - 1):
        attend_block(b)
    step(1, 2) if outer > 2 else None
    step0(2)
    halo_wait(kv, WINDOW, 0)
    attend_block(0)
    attend_block(blocks - 1)
    for k in range(3, outer):
        step(1, k)
    take_all(1)

    step0_partner(2)
    for n in range(items // tile):
        rows = pl.ds(n * tile, tile)
        inner = pl.ds(edge + n * tile, tile)
        conv_input = project(b_buf, rows, slice(0, cw))
        before = project(b_buf, rows, slice(2 * cw, 3 * cw))
        sec[inner, :] = (before * conv_input).astype(bf16)
        if n == 0:
            step(2, 1)
    halo(sec, edge, 2)
    if outer > 2:
        step(2, 2)
    for n in range(items // tile):
        rows = pl.ds(n * tile, tile)
        proj[rows, :] = project(b_buf, rows, slice(cw, 2 * cw))
    halo_wait(sec, edge, 2)
    full = sec[...].astype(f32)
    taps = taps_ref[...].astype(f32)
    length = full.shape[0]
    conv = (
        pltpu.roll(full, 1, 0) * taps[0:1]
        + full * taps[1:2]
        + pltpu.roll(full, length - 1, 0) * taps[2:3]
    )
    mix[:, qw:] = (proj[...] * conv[edge : edge + items]).astype(bf16)

    width = c_buf.shape[2]

    core = lax.rem(t, 2)

    def produce(owner, slot):
        mine = lax.rem(owner, 2) == core

        def one(n, carry):
            rows = pl.ds(pl.multiple_of(n * tile, tile), tile)
            x = mix[rows, :]
            for j in range(2):
                cols = slice(j * width, (j + 1) * width)
                y = jnp.dot(x, c_buf[2 * owner + j], preferred_element_type=f32)

                @pl.when(owner == t)
                def _():
                    loc[rows, cols] = y

                @pl.when(mine & (owner != t))
                def _():
                    pre[slot, rows, cols] = y

                @pl.when(jnp.logical_not(mine))
                def _():
                    stage[owner, rows, cols] = y.astype(bf16)
            return carry

        lax.fori_loop(0, items // tile, one, 0)

    def pair_wait(owner):
        ref = pair.at[lax.div(owner, 2)]
        remote(ref, ref, rs_send.at[0], pair_recv.at[lax.div(owner, 2)], (s, sibling)).wait_recv()

    def give(cond, owner, slot):
        pl.when(cond)(lambda: produce(owner, slot))
        post(cond & (lax.rem(owner, 2) != core), stage.at[owner], pair.at[lax.div(owner, 2)],
             rs_send.at[owner], pair_recv.at[lax.div(owner, 2)], (s, sibling))

    def finish(cond, owner, slot):
        active = cond & (lax.rem(owner, 2) == core) & (owner != t)

        @pl.when(active)
        def _():
            pair_wait(owner)
            stage[owner] = (pre[slot] + pair[lax.div(owner, 2)].astype(f32)).astype(bf16)

        post(active, stage.at[owner], rbuf.at[lax.div(t, 2)], rs_send.at[owner],
             rs_recv.at[lax.div(t, 2)], (s, owner))

    give(always, o, 0)
    finish(always, o, 0)
    for k in range(1, outer):
        if k > 2:
            step(2, k)
        pl.when(o >= k)(lambda: take(2, k, True))
        give(o >= k, o - k, 0)
        pl.when(o + k < outer)(lambda: take(2, k, False))
        give(o + k < outer, o + k, 1)
        finish(o >= k, o - k, 0)
        finish(o + k < outer, o + k, 1)

    pair_wait(t)
    summed = loc[...] + pair[lax.div(t, 2)].astype(f32)
    for far in across:
        slot = lax.div(far, 2)
        remote(rbuf.at[slot], rbuf.at[slot], rs_send.at[0], rs_recv.at[slot], (s, far)).wait_recv()
        summed = summed + rbuf[slot].astype(f32)
    loc[...] = summed
    lane = lax.broadcasted_iota(jnp.int32, (items, 128), 1)
    both = jnp.where(
        lane == 0, jnp.sum(summed, 1, keepdims=True), jnp.sum(summed * summed, 1, keepdims=True)
    )
    my_stat[...] = jnp.transpose(both)[:8]
    for d in range(1, tp):
        dst = lax.rem(t + d, tp)
        post(always, my_stat, stats.at[t], st_send.at[d], st_recv.at[t], (s, dst))
    total = my_stat[...]
    for d in range(1, tp):
        src = lax.rem(t + d, tp)
        remote(stats.at[src], stats.at[src], st_send.at[0], st_recv.at[src], (s, src)).wait_recv()
        total = total + stats[src]
    total = total * (1.0 / (tp * out_ref.shape[1]))
    total = jnp.transpose(jnp.concatenate([total] * 16, 0))
    mean = total[:, 0:1]
    spread = total[:, 1:2] - mean * mean
    out_ref[...] = ((loc[...] - mean) * lax.rsqrt(spread + EPS) * gain_ref[...]).astype(bf16)

    for cond, args in sends:
        pl.when(cond)(lambda args=args: remote(*args).wait_send())


def small_tables(offset, items):
    half = HEAD_SIZE // 2
    inverse = THETA ** (-jnp.arange(0, half, 2, dtype=jnp.float32) / half)
    inverse = jnp.concatenate([inverse] * 4)[None]
    row = (offset // GRID + jnp.arange(items // GRID, dtype=jnp.int32)).astype(jnp.float32)
    column = jnp.arange(GRID, dtype=jnp.int32).astype(jnp.float32)
    row, column = row[:, None] * inverse, column[:, None] * inverse
    return jnp.cos(row), jnp.sin(row), jnp.cos(column), jnp.sin(column)


def body(
    sizes, tokens, query_weight, key_projection, value_projection, conv_in_weight, conv_gate_out,
    conv_gate_in, conv_taps, head_sink_logit, out_attn_weight, out_conv_weight, out_gain,
):
    span, tp = sizes["sp"], sizes["tp"]
    items, features = tokens.shape
    depth = query_weight.shape[0]
    group = query_weight.shape[1] // HEAD_SIZE
    fits = (
        span == 2 * tp and tp % 2 == 0 and depth % 128 == 0 and features == 2 * depth
        and out_attn_weight.shape[1] % 128 == 0 and items % (2 * WINDOW) == 0
        and key_projection.shape[1] == HEAD_SIZE and conv_in_weight.shape[1] % 128 == 0
        and out_attn_weight.shape[0] == out_conv_weight.shape[0]
    )
    if not fits:
        return plain_body(
            tokens, query_weight, key_projection, value_projection, conv_in_weight, conv_gate_out,
            conv_gate_in, conv_taps, head_sink_logit, out_attn_weight, out_conv_weight, out_gain,
        )
    tables = small_tables(lax.axis_index("sp") * items, items)
    outer = span // 2
    f32, bf16 = jnp.float32, jnp.bfloat16
    qw, kw, cw = query_weight.shape[1], key_projection.shape[1], conv_in_weight.shape[1]
    mixer = out_attn_weight.shape[0] + out_conv_weight.shape[0]
    own_width = out_gain.shape[0]
    dma = pltpu.SemaphoreType.DMA
    anywhere = pl.BlockSpec(memory_space=pl.ANY)
    vmem = pl.BlockSpec(memory_space=pltpu.VMEM)
    smem = pl.BlockSpec(memory_space=pltpu.SMEM)
    return pl.pallas_call(
        functools.partial(fused_kernel, outer, tp),
        out_shape=jax.ShapeDtypeStruct((items, own_width), bf16),
        in_specs=[anywhere] * 9 + [vmem, smem, vmem] + [vmem] * 4,
        out_specs=vmem,
        scratch_shapes=[
            pltpu.VMEM((tp, items, features), bf16),
            pltpu.VMEM((span, depth, qw + 2 * kw), bf16),
            pltpu.VMEM((span, depth, 3 * cw), bf16),
            pltpu.VMEM((span, mixer, out_attn_weight.shape[1]), bf16),
            pltpu.VMEM((items, qw), bf16),
            pltpu.VMEM((items + 2 * WINDOW, 2 * kw), bf16),
            pltpu.VMEM((items, cw), f32),
            pltpu.VMEM((items + 32, cw), bf16),
            pltpu.VMEM((items, mixer), bf16),
            pltpu.VMEM((tp, items, own_width), bf16),
            pltpu.VMEM((tp // 2, items, own_width), bf16),
            pltpu.VMEM((tp // 2, items, own_width), bf16),
            pltpu.VMEM((2, items, own_width), f32),
            pltpu.VMEM((items, own_width), f32),
            pltpu.VMEM((8, items), f32),
            pltpu.VMEM((tp, 8, items), f32),
            dma((9,)),
            dma((3, 4, span, 2)),
            dma((3, span, 2)),
            dma((tp,)),
            dma((tp,)),
            dma((4,)),
            dma((4,)),
            dma((tp,)),
            dma((tp,)),
            dma((tp // 2,)),
            dma((tp,)),
            dma((tp,)),
        ],
        compiler_params=pltpu.CompilerParams(
            collective_id=0, has_side_effects=True, vmem_limit_bytes=60 * 2**20
        ),
    )(
        tokens, query_weight, key_projection, value_projection, conv_in_weight, conv_gate_out,
        conv_gate_in, out_attn_weight, out_conv_weight, conv_taps, head_sink_logit,
        out_gain[None], *tables,
    )


def solution(mesh):
    return jax.shard_map(
        functools.partial(body, dict(mesh.shape)),
        mesh=mesh,
        in_specs=(
            P("sp", "tp"),
            P("sp", "tp"),
            P("sp", "tp"),
            P("sp", "tp"),
            P("sp", "tp"),
            P("sp", "tp"),
            P("sp", "tp"),
            P(None, "tp"),
            P("tp"),
            P("tp", "sp"),
            P("tp", "sp"),
            P("tp"),
        ),
        out_specs=P("sp", "tp"),
        check_vma=False,
    )
```

```python
import functools

import jax
import jax.numpy as jnp
from jax import lax
from jax.experimental import pallas as pl
from jax.experimental.pallas import tpu as pltpu
from jax.sharding import PartitionSpec as P

HEAD_SIZE = 128
WINDOW = 128
GRID = 64


NEG_BIG = -1e30
THETA = 10000.0
EPS = 1e-05


def with_halo(block, sides, width):
    for axis, dim in sides:
        count = lax.axis_size(axis)
        forward = [(i, i + 1) for i in range(count - 1)]
        backward = [(target, source) for source, target in forward]
        low = lax.ppermute(
            lax.slice_in_dim(block, block.shape[dim] - width, None, axis=dim), axis, forward
        )
        high = lax.ppermute(lax.slice_in_dim(block, 0, width, axis=dim), axis, backward)
        block = jnp.concatenate([low, block, high], axis=dim)
    return block


def rope_tables(positions):
    row = (positions // GRID).astype(jnp.float32)
    column = (positions % GRID).astype(jnp.float32)
    half = HEAD_SIZE // 2
    inverse = THETA ** (-jnp.arange(0, half, 2, dtype=jnp.float32) / half)
    angle_row = row[:, None] * inverse
    angle_col = column[:, None] * inverse
    angles = jnp.concatenate([angle_row, angle_row, angle_col, angle_col], -1)
    return (jnp.cos(angles)[:, None, :], jnp.sin(angles)[:, None, :])


def rotate(vectors, cosine, sine):
    first, second, third, fourth = jnp.split(vectors, 4, axis=-1)
    turned = jnp.concatenate([-second, first, -fourth, third], -1)
    return vectors * cosine + turned * sine


def attend(query_vectors, paired, head_sink_logit, offset, total_tokens):
    item_count = query_vectors.shape[0]
    kv_heads = paired.shape[1] // (2 * HEAD_SIZE)
    head_group = query_vectors.shape[1] // (kv_heads * HEAD_SIZE)
    blocks = item_count // WINDOW
    padded = with_halo(paired, (("sp", 0),), WINDOW)
    shaped = padded.reshape(blocks + 2, WINDOW, paired.shape[1])
    banded = jnp.concatenate([shaped[:-2], shaped[1:-1], shaped[2:]], axis=1)
    banded = banded.reshape(blocks, 3 * WINDOW, 2, kv_heads, HEAD_SIZE)
    key_band = banded[:, :, 0]
    value_band = banded[:, :, 1]
    query_blocks = query_vectors.reshape(blocks, WINDOW, kv_heads, head_group, HEAD_SIZE)
    scores = jnp.einsum(
        "nqhgd,nkhd->nhgqk", query_blocks, key_band, preferred_element_type=jnp.float32
    ) * HEAD_SIZE ** (-0.5)
    block_start = offset + jnp.arange(blocks, dtype=jnp.int32)[:, None] * WINDOW
    query_pos = block_start + jnp.arange(WINDOW, dtype=jnp.int32)[None, :]
    key_pos = block_start - WINDOW + jnp.arange(3 * WINDOW, dtype=jnp.int32)[None, :]
    distance = key_pos[:, None, :] - query_pos[:, :, None]
    valid = (
        (jnp.abs(distance) <= WINDOW)
        & (key_pos[:, None, :] >= 0)
        & (key_pos[:, None, :] < total_tokens)
    )
    scores = jnp.where(valid[:, None, None], scores, NEG_BIG)
    sink_col = head_sink_logit.reshape(1, kv_heads, head_group, 1, 1)
    top = jnp.maximum(jnp.max(scores, -1, keepdims=True), sink_col)
    weights = jnp.exp(scores - top)
    denominator = jnp.sum(weights, -1, keepdims=True) + jnp.exp(sink_col - top)
    probs = (weights / denominator).astype(jnp.bfloat16)
    mixed_heads = jnp.einsum(
        "nhgqk,nkhd->nqhgd", probs, value_band, preferred_element_type=jnp.float32
    )
    return mixed_heads.reshape(item_count, kv_heads * head_group * HEAD_SIZE).astype(jnp.bfloat16)


def convolve(gate_before, conv_input, gate_after, conv_taps):
    sectioned = (gate_before * conv_input).astype(jnp.bfloat16)
    bordered = with_halo(sectioned, (("sp", 0),), 1)
    taps = conv_taps.astype(jnp.float32)
    conv_mix = bordered[:-2] * taps[0] + bordered[1:-1] * taps[1] + bordered[2:] * taps[2]
    return (gate_after * conv_mix).astype(jnp.bfloat16)


def plain_body(
    tokens,
    query_weight,
    key_projection,
    value_projection,
    conv_in_weight,
    conv_gate_out,
    conv_gate_in,
    conv_taps,
    head_sink_logit,
    out_attn_weight,
    out_conv_weight,
    out_gain,
):
    whole = lax.all_gather(tokens, "tp", axis=1, tiled=True)
    item_count = whole.shape[0]
    offset = lax.axis_index("sp") * item_count
    total_tokens = item_count * lax.axis_size("sp")
    positions = offset + jnp.arange(item_count, dtype=jnp.int32)
    cosine, sine = rope_tables(positions)
    pieces = (
        lax.all_gather(query_weight, "sp", axis=0, tiled=True),
        lax.all_gather(key_projection, "sp", axis=0, tiled=True),
        lax.all_gather(value_projection, "sp", axis=0, tiled=True),
        lax.all_gather(conv_in_weight, "sp", axis=0, tiled=True),
        lax.all_gather(conv_gate_out, "sp", axis=0, tiled=True),
        lax.all_gather(conv_gate_in, "sp", axis=0, tiled=True),
    )
    query_raw, key_unrotated, value_raw, conv_input, gate_after, gate_before = tuple(
        (jnp.dot(whole, piece, preferred_element_type=jnp.float32) for piece in pieces)
    )
    query_vectors = (
        rotate(query_raw.reshape(item_count, -1, HEAD_SIZE), cosine, sine)
        .reshape(item_count, -1)
        .astype(jnp.bfloat16)
    )
    key_rows = (
        rotate(key_unrotated.reshape(item_count, -1, HEAD_SIZE), cosine, sine)
        .reshape(item_count, -1)
        .astype(jnp.bfloat16)
    )
    paired = jnp.concatenate([key_rows, value_raw.astype(jnp.bfloat16)], 1)
    attention_out = attend(query_vectors, paired, head_sink_logit, offset, total_tokens)
    conv_out = convolve(gate_before, conv_input, gate_after, conv_taps)
    mixer_rows = jnp.concatenate([attention_out, conv_out], 1)
    stacked = jnp.concatenate([out_attn_weight, out_conv_weight], 0)
    own_width = out_gain.shape[0]
    partial_sums = jnp.dot(
        mixer_rows,
        lax.all_gather(stacked, "sp", axis=1, tiled=True),
        preferred_element_type=jnp.float32,
    )
    summed = lax.psum_scatter(
        partial_sums.astype(jnp.bfloat16), "tp", scatter_dimension=1, tiled=True
    ).astype(jnp.float32)
    full_width = own_width * lax.axis_size("tp")
    first_sum, square_sum = lax.psum((jnp.sum(summed, 1), jnp.sum(summed * summed, 1)), "tp")
    mean = first_sum / full_width
    spread = square_sum / full_width - mean * mean
    normed = (summed - mean[:, None]) * lax.rsqrt(spread[:, None] + EPS) * out_gain
    return normed.astype(jnp.bfloat16)


def fused_kernel(
    outer, tp, tokens_ref, wq_ref, wk_ref, wv_ref, wi_ref, wgo_ref, wgi_ref, wa_ref, wc_ref,
    taps_ref, sink_ref, gain_ref, cosr_ref, sinr_ref, cosc_ref, sinc_ref, out_ref,
    tok, a_buf, b_buf, c_buf, q_buf, kv, proj, sec, mix, stage, rbuf, pair, pre, loc, my_stat, stats,
    local_sem, w_send, w_recv, t_send, t_recv, halo_send, halo_recv, rs_send, rs_recv, pair_recv,
    st_send, st_recv,
):
    f32, bf16 = jnp.float32, jnp.bfloat16
    s, t = lax.axis_index("sp"), lax.axis_index("tp")
    span = 2 * outer
    o, i = lax.div(s, 2), lax.rem(s, 2)
    odd = lax.rem(o, 2)
    mate = o + 1 - 2 * odd
    partner = 2 * o + 1 - i
    items = tokens_ref.shape[0]
    blocks = items // WINDOW
    edge = 16
    sends = []
    always = s >= 0

    def remote(src, dst, send_sem, recv_sem, dev):
        return pltpu.make_async_remote_copy(
            src_ref=src, dst_ref=dst, send_sem=send_sem, recv_sem=recv_sem,
            device_id=dev, device_id_type=pl.DeviceIdType.MESH,
        )

    def post(cond, *args):
        def run():
            remote(*args).start()

        pl.when(cond)(run)
        sends.append((cond, args))

    half_c = wa_ref.shape[0]
    qw, kw = wq_ref.shape[1], wk_ref.shape[1]
    cw = wi_ref.shape[1]
    own = [
        (tokens_ref, tok.at[t]),
        (wq_ref, a_buf.at[s, :, pl.ds(0, qw)]),
        (wk_ref, a_buf.at[s, :, pl.ds(qw, kw)]),
        (wv_ref, a_buf.at[s, :, pl.ds(qw + kw, kw)]),
        (wi_ref, b_buf.at[s, :, pl.ds(0, cw)]),
        (wgo_ref, b_buf.at[s, :, pl.ds(cw, cw)]),
        (wgi_ref, b_buf.at[s, :, pl.ds(2 * cw, cw)]),
        (wa_ref, c_buf.at[s, pl.ds(0, half_c)]),
        (wc_ref, c_buf.at[s, pl.ds(half_c, half_c)]),
    ]
    local = [
        pltpu.make_async_copy(a, b, local_sem.at[n]) for n, (a, b) in enumerate(own)
    ]
    for copy in local:
        copy.start()

    barrier = pltpu.get_barrier_semaphore()
    greet = [(s + 1 < span, (s + 1, t)), (s > 0, (s - 1, t)),
             (o + 1 < outer, (s + 2, t)), (o > 0, (s - 2, t))]
    greet += [(always, (s, lax.rem(t + d, tp))) for d in range(1, tp)]
    for cond, dev in greet:
        @pl.when(cond)
        def _(dev=dev):
            pl.semaphore_signal(barrier, inc=1, device_id=dev, device_id_type=pl.DeviceIdType.MESH)
    pl.semaphore_wait(barrier, sum(cond.astype(jnp.int32) for cond, dev in greet))

    bufs = (a_buf, b_buf, c_buf)

    def unit(p, piece, h):
        rows = bufs[p].shape[1] // 2
        return bufs[p].at[piece, pl.ds(h * rows, rows)]

    def send(p, piece, h, d, dev, cond):
        ref = unit(p, piece, h)
        post(cond, ref, ref, w_send.at[p, d, piece, h], w_recv.at[p, piece, h], (dev, t))

    def recv(p, piece, h):
        ref = unit(p, piece, h)
        remote(ref, ref, w_send.at[p, 0, piece, h], w_recv.at[p, piece, h], (partner, t)).wait_recv()

    def step0(p):
        for h in range(2):
            send(p, s, h, 0, s + 2, o + 1 < outer)
            send(p, s, h, 1, s - 2, o > 0)
            send(p, s, h, 2, partner, always)

    def step0_partner(p):
        recv(p, partner, 0)
        recv(p, partner, 1)
        send(p, partner, 1, 3, 2 * mate + i, always)

    def step(p, k):
        for h in range(2):
            low, high = s - 2 * k, s + 2 * k
            has_low, has_high = o >= k, o + k < outer
            pl.when(has_low)(lambda: recv(p, low, h))
            send(p, low, h, 0, s + 2, has_low & (o + 1 < outer))
            skip = h == 1 and k == 1
            send(p, low, h, 2, partner, (has_low & (odd == 0)) if skip else has_low)
            pl.when(has_high)(lambda: recv(p, high, h))
            send(p, high, h, 1, s - 2, has_high & (o > 0))
            send(p, high, h, 2, partner, (has_high & (odd == 1)) if skip else has_high)

    def take(p, k, low):
        base = partner - 2 * k if low else partner + 2 * k
        for h in range(2):
            recv(p, base, h)

    def take_all(p):
        for k in range(1, outer):
            pl.when(o >= k)(lambda: take(p, k, True))
            pl.when(o + k < outer)(lambda: take(p, k, False))

    for copy in local[:4]:
        copy.wait()
    sibling = t + 1 - 2 * lax.rem(t, 2)
    post(always, tok.at[t], tok.at[t], t_send.at[0], t_recv.at[t], (s, sibling))
    across = [lax.rem(t + 2 * d, tp) for d in range(1, tp // 2)]
    for n, far in enumerate(across):
        post(always, tok.at[t], tok.at[t], t_send.at[1 + n], t_recv.at[t], (s, far))

    def wait_tok(src):
        remote(tok.at[src], tok.at[src], t_send.at[0], t_recv.at[src], (s, sibling)).wait_recv()

    step0(0)
    for copy in local[4:]:
        copy.wait()
    step0_partner(0)
    step(0, 1)
    step0(1)
    for k in range(2, outer):
        step(0, k)
    for n, far in enumerate(across):
        wait_tok(far)
        post(always, tok.at[far], tok.at[far], t_send.at[tp // 2 + n], t_recv.at[far], (s, sibling))
    wait_tok(sibling)
    for far in across:
        wait_tok(far + 1 - 2 * lax.rem(far, 2))
    take_all(0)

    tile = 256
    depth = a_buf.shape[1]
    per = tok.shape[2] // depth

    def project(buf, rows, cols):
        total = None
        for piece in range(span):
            lane = (piece % per) * depth
            term = jnp.dot(
                tok[piece // per, rows, lane : lane + depth], buf[piece, :, cols],
                preferred_element_type=f32,
            )
            total = term if total is None else total + term
        return total

    lane_row = lax.broadcasted_iota(jnp.int32, (1, HEAD_SIZE), 1)
    first_half = lax.rem(lane_row, HEAD_SIZE // 2) < HEAD_SIZE // 4
    left_lanes = (lane_row < HEAD_SIZE // 2)[None]
    for n in range(items // tile):
        rows = pl.ds(n * tile, tile)
        grid_rows = tile // GRID

        def table(row_ref, col_ref):
            r = row_ref[pl.ds(n * grid_rows, grid_rows), :][:, None, :]
            c = col_ref[...][None]
            r = jnp.broadcast_to(r, (grid_rows, GRID, HEAD_SIZE))
            c = jnp.broadcast_to(c, (grid_rows, GRID, HEAD_SIZE))
            return jnp.where(left_lanes, r, c).reshape(tile, HEAD_SIZE)

        cosine = table(cosr_ref, cosc_ref)
        sine = table(sinr_ref, sinc_ref)
        sine = jnp.where(first_half, -sine, sine)
        raw = project(a_buf, rows, slice(None))

        def turn(u):
            other = jnp.where(
                first_half, pltpu.roll(u, HEAD_SIZE - HEAD_SIZE // 4, 1), pltpu.roll(u, HEAD_SIZE // 4, 1)
            )
            return (u * cosine + other * sine).astype(bf16)

        for g in range(qw // HEAD_SIZE):
            cols = slice(g * HEAD_SIZE, (g + 1) * HEAD_SIZE)
            q_buf[rows, cols] = turn(raw[:, cols])
        inner = pl.ds(WINDOW + n * tile, tile)
        kv[inner, :kw] = turn(raw[:, qw : qw + kw])
        kv[inner, kw:] = raw[:, qw + kw :].astype(bf16)

    has_left, has_right = s > 0, s + 1 < span

    def halo(ref, width, base):
        last = ref.shape[0] - width
        post(has_right, ref.at[pl.ds(last - width, width)], ref.at[pl.ds(0, width)],
             halo_send.at[base], halo_recv.at[base], (s + 1, t))
        post(has_left, ref.at[pl.ds(width, width)], ref.at[pl.ds(last, width)],
             halo_send.at[base + 1], halo_recv.at[base + 1], (s - 1, t))

    def halo_wait(ref, width, base):
        last = ref.shape[0] - width
        for n, (cond, start) in enumerate(((has_left, 0), (has_right, last))):
            dst = ref.at[pl.ds(start, width)]

            @pl.when(cond)
            def _():
                remote(dst, dst, halo_send.at[base + n], halo_recv.at[base + n], (partner, t)).wait_recv()

            @pl.when(jnp.logical_not(cond))
            def _():
                ref[pl.ds(start, width), :] = jnp.zeros((width, ref.shape[1]), ref.dtype)

    halo(kv, WINDOW, 0)

    group = qw // HEAD_SIZE
    shape = (group * WINDOW, 3 * WINDOW)

    def attend_block(b):
        rows = pl.ds(b * WINDOW, WINDOW)
        band = pl.ds(b * WINDOW, 3 * WINDOW)
        q = jnp.concatenate(
            [q_buf[rows, g * HEAD_SIZE : (g + 1) * HEAD_SIZE] for g in range(group)], 0
        )
        scores = lax.dot_general(
            q, kv[band, :kw], (((1,), (1,)), ((), ())), preferred_element_type=f32
        ) * HEAD_SIZE ** (-0.5)
        row = lax.broadcasted_iota(jnp.int32, shape, 0)
        col = lax.broadcasted_iota(jnp.int32, shape, 1)
        gap = col - WINDOW - lax.rem(row, WINDOW)
        position = s * items + (b - 1) * WINDOW + col
        valid = (jnp.abs(gap) <= WINDOW) & (position >= 0) & (position < items * span)
        scores = jnp.where(valid, scores, NEG_BIG)
        head = lax.broadcasted_iota(jnp.int32, (group * WINDOW, 1), 0) // WINDOW
        sink = jnp.zeros((group * WINDOW, 1), f32)
        for g in range(group):
            sink = jnp.where(head == g, sink_ref[g], sink)
        top = jnp.maximum(jnp.max(scores, -1, keepdims=True), sink)
        weights = jnp.exp(scores - top)
        denominator = jnp.sum(weights, -1, keepdims=True) + jnp.exp(sink - top)
        probs = (weights / denominator).astype(bf16)
        mixed = jnp.dot(probs, kv[band, kw:], preferred_element_type=f32).astype(bf16)
        for g in range(group):
            mix[rows, g * HEAD_SIZE : (g + 1) * HEAD_SIZE] = mixed[g * WINDOW : (g + 1) * WINDOW]

    def add(piece, first=False):
        source, lane = lax.div(piece, per), lax.rem(piece, per) * depth

        def one(n, carry):
            rows = pl.ds(pl.multiple_of(n * tile, tile), tile)
            x = tok[source, rows, pl.ds(pl.multiple_of(lane, depth), depth)]
            term = jnp.dot(x, b_buf[piece], preferred_element_type=f32)
            proj[rows, :] = term if first else proj[rows, :] + term
            return carry

        lax.fori_loop(0, items // tile, one, 0)

    def add_pair(k, base):
        pl.when(o >= k)(lambda: add(base - 2 * k))
        pl.when(o + k < outer)(lambda: add(base + 2 * k))

    def take_pair(k):
        pl.when(o >= k)(lambda: take(1, k, True))
        pl.when(o + k < outer)(lambda: take(1, k, False))
        add_pair(k, partner)

    step0_partner(1)
    step(1, 1)
    add(s, True)
    add(partner)
    add_pair(1, s)
    for b in range(1, blocks - 1):
        attend_block(b)
    step(1, 2) if outer > 2 else None
    step0(2)
    halo_wait(kv, WINDOW, 0)
    attend_block(0)
    attend_block(blocks - 1)
    for k in range(3, outer):
        step(1, k)
        take_pair(k - 2)
        add_pair(k - 1, s)
    take_pair(outer - 2)
    add_pair(outer - 1, s)
    step0_partner(2)
    step(2, 1)
    take_pair(outer - 1)

    sec[edge : edge + items, :] = (proj[:, 2 * cw :] * proj[:, :cw]).astype(bf16)
    halo(sec, edge, 2)
    if outer > 2:
        step(2, 2)
    halo_wait(sec, edge, 2)
    full = sec[...].astype(f32)
    taps = taps_ref[...].astype(f32)
    length = full.shape[0]
    conv = (
        pltpu.roll(full, 1, 0) * taps[0:1]
        + full * taps[1:2]
        + pltpu.roll(full, length - 1, 0) * taps[2:3]
    )
    mix[:, qw:] = (proj[:, cw : 2 * cw] * conv[edge : edge + items]).astype(bf16)

    width = c_buf.shape[2]

    core = lax.rem(t, 2)

    def produce(owner, slot):
        mine = lax.rem(owner, 2) == core

        def one(n, carry):
            rows = pl.ds(pl.multiple_of(n * tile, tile), tile)
            x = mix[rows, :]
            for j in range(2):
                cols = slice(j * width, (j + 1) * width)
                y = jnp.dot(x, c_buf[2 * owner + j], preferred_element_type=f32)

                @pl.when(owner == t)
                def _():
                    loc[rows, cols] = y

                @pl.when(mine & (owner != t))
                def _():
                    pre[slot, rows, cols] = y

                @pl.when(jnp.logical_not(mine))
                def _():
                    stage[owner, rows, cols] = y.astype(bf16)
            return carry

        lax.fori_loop(0, items // tile, one, 0)

    def pair_wait(owner):
        ref = pair.at[lax.div(owner, 2)]
        remote(ref, ref, rs_send.at[0], pair_recv.at[lax.div(owner, 2)], (s, sibling)).wait_recv()

    def give(cond, owner, slot):
        pl.when(cond)(lambda: produce(owner, slot))
        post(cond & (lax.rem(owner, 2) != core), stage.at[owner], pair.at[lax.div(owner, 2)],
             rs_send.at[owner], pair_recv.at[lax.div(owner, 2)], (s, sibling))

    def finish(cond, owner, slot):
        active = cond & (lax.rem(owner, 2) == core) & (owner != t)

        @pl.when(active)
        def _():
            pair_wait(owner)
            stage[owner] = (pre[slot] + pair[lax.div(owner, 2)].astype(f32)).astype(bf16)

        post(active, stage.at[owner], rbuf.at[lax.div(t, 2)], rs_send.at[owner],
             rs_recv.at[lax.div(t, 2)], (s, owner))

    give(always, o, 0)
    finish(always, o, 0)
    for k in range(1, outer):
        if k > 2:
            step(2, k)
        pl.when(o >= k)(lambda: take(2, k, True))
        give(o >= k, o - k, 0)
        pl.when(o + k < outer)(lambda: take(2, k, False))
        give(o + k < outer, o + k, 1)
        finish(o >= k, o - k, 0)
        finish(o + k < outer, o + k, 1)

    pair_wait(t)
    summed = loc[...] + pair[lax.div(t, 2)].astype(f32)
    for far in across:
        slot = lax.div(far, 2)
        remote(rbuf.at[slot], rbuf.at[slot], rs_send.at[0], rs_recv.at[slot], (s, far)).wait_recv()
        summed = summed + rbuf[slot].astype(f32)
    loc[...] = summed
    lane = lax.broadcasted_iota(jnp.int32, (items, 128), 1)
    both = jnp.where(
        lane == 0, jnp.sum(summed, 1, keepdims=True), jnp.sum(summed * summed, 1, keepdims=True)
    )
    my_stat[...] = jnp.transpose(both)[:8]
    for d in range(1, tp):
        dst = lax.rem(t + d, tp)
        post(always, my_stat, stats.at[t], st_send.at[d], st_recv.at[t], (s, dst))
    total = my_stat[...]
    for d in range(1, tp):
        src = lax.rem(t + d, tp)
        remote(stats.at[src], stats.at[src], st_send.at[0], st_recv.at[src], (s, src)).wait_recv()
        total = total + stats[src]
    total = total * (1.0 / (tp * out_ref.shape[1]))
    total = jnp.transpose(jnp.concatenate([total] * 16, 0))
    mean = total[:, 0:1]
    spread = total[:, 1:2] - mean * mean
    out_ref[...] = ((loc[...] - mean) * lax.rsqrt(spread + EPS) * gain_ref[...]).astype(bf16)

    for cond, args in sends:
        pl.when(cond)(lambda args=args: remote(*args).wait_send())


def small_tables(offset, items):
    half = HEAD_SIZE // 2
    inverse = THETA ** (-jnp.arange(0, half, 2, dtype=jnp.float32) / half)
    inverse = jnp.concatenate([inverse] * 4)[None]
    row = (offset // GRID + jnp.arange(items // GRID, dtype=jnp.int32)).astype(jnp.float32)
    column = jnp.arange(GRID, dtype=jnp.int32).astype(jnp.float32)
    row, column = row[:, None] * inverse, column[:, None] * inverse
    return jnp.cos(row), jnp.sin(row), jnp.cos(column), jnp.sin(column)


def body(
    sizes, tokens, query_weight, key_projection, value_projection, conv_in_weight, conv_gate_out,
    conv_gate_in, conv_taps, head_sink_logit, out_attn_weight, out_conv_weight, out_gain,
):
    span, tp = sizes["sp"], sizes["tp"]
    items, features = tokens.shape
    depth = query_weight.shape[0]
    group = query_weight.shape[1] // HEAD_SIZE
    fits = (
        span == 2 * tp and tp % 2 == 0 and depth % 128 == 0 and features == 2 * depth
        and out_attn_weight.shape[1] % 128 == 0 and items % (2 * WINDOW) == 0
        and key_projection.shape[1] == HEAD_SIZE and conv_in_weight.shape[1] % 128 == 0
        and out_attn_weight.shape[0] == out_conv_weight.shape[0] and tp > 2
    )
    if not fits:
        return plain_body(
            tokens, query_weight, key_projection, value_projection, conv_in_weight, conv_gate_out,
            conv_gate_in, conv_taps, head_sink_logit, out_attn_weight, out_conv_weight, out_gain,
        )
    tables = small_tables(lax.axis_index("sp") * items, items)
    outer = span // 2
    f32, bf16 = jnp.float32, jnp.bfloat16
    qw, kw, cw = query_weight.shape[1], key_projection.shape[1], conv_in_weight.shape[1]
    mixer = out_attn_weight.shape[0] + out_conv_weight.shape[0]
    own_width = out_gain.shape[0]
    dma = pltpu.SemaphoreType.DMA
    anywhere = pl.BlockSpec(memory_space=pl.ANY)
    vmem = pl.BlockSpec(memory_space=pltpu.VMEM)
    smem = pl.BlockSpec(memory_space=pltpu.SMEM)
    return pl.pallas_call(
        functools.partial(fused_kernel, outer, tp),
        out_shape=jax.ShapeDtypeStruct((items, own_width), bf16),
        in_specs=[anywhere] * 9 + [vmem, smem, vmem] + [vmem] * 4,
        out_specs=vmem,
        scratch_shapes=[
            pltpu.VMEM((tp, items, features), bf16),
            pltpu.VMEM((span, depth, qw + 2 * kw), bf16),
            pltpu.VMEM((span, depth, 3 * cw), bf16),
            pltpu.VMEM((span, mixer, out_attn_weight.shape[1]), bf16),
            pltpu.VMEM((items, qw), bf16),
            pltpu.VMEM((items + 2 * WINDOW, 2 * kw), bf16),
            pltpu.VMEM((items, 3 * cw), f32),
            pltpu.VMEM((items + 32, cw), bf16),
            pltpu.VMEM((items, mixer), bf16),
            pltpu.VMEM((tp, items, own_width), bf16),
            pltpu.VMEM((tp // 2, items, own_width), bf16),
            pltpu.VMEM((tp // 2, items, own_width), bf16),
            pltpu.VMEM((2, items, own_width), f32),
            pltpu.VMEM((items, own_width), f32),
            pltpu.VMEM((8, items), f32),
            pltpu.VMEM((tp, 8, items), f32),
            dma((9,)),
            dma((3, 4, span, 2)),
            dma((3, span, 2)),
            dma((tp,)),
            dma((tp,)),
            dma((4,)),
            dma((4,)),
            dma((tp,)),
            dma((tp,)),
            dma((tp // 2,)),
            dma((tp,)),
            dma((tp,)),
        ],
        compiler_params=pltpu.CompilerParams(
            collective_id=0, has_side_effects=True, vmem_limit_bytes=60 * 2**20
        ),
    )(
        tokens, query_weight, key_projection, value_projection, conv_in_weight, conv_gate_out,
        conv_gate_in, out_attn_weight, out_conv_weight, conv_taps, head_sink_logit,
        out_gain[None], *tables,
    )


def solution(mesh):
    return jax.shard_map(
        functools.partial(body, dict(mesh.shape)),
        mesh=mesh,
        in_specs=(
            P("sp", "tp"),
            P("sp", "tp"),
            P("sp", "tp"),
            P("sp", "tp"),
            P("sp", "tp"),
            P("sp", "tp"),
            P("sp", "tp"),
            P(None, "tp"),
            P("tp"),
            P("tp", "sp"),
            P("tp", "sp"),
            P("tp"),
        ),
        out_specs=P("sp", "tp"),
        check_vma=False,
    )
```
